32 devices in a mesh: grp: 2 (over y), sp: 4 (over z), dp: 4 (over x, core).
Axes of the slice: x: 2, y: 2, z: 4, core: 2. Of those that a mesh axis runs over, the one named last changes fastest.
Arguments:
- query_rows: bfloat16 [8, 512, 2048], P(('grp', 'dp'), 'sp'), parts along dimension 0, may hold values from -6 to 6
- key_rows: bfloat16 [8, 512, 2048], P(('grp', 'dp'), 'sp'), parts along dimension 0, may hold values from -6 to 6
- value_rows: bfloat16 [8, 512, 2048], P(('grp', 'dp'), 'sp'), parts along dimension 0, may hold values from -6 to 6
- query_gain: float32 [64], replicated, may hold values from 1.1 to 7
- key_gain: float32 [64], replicated, may hold values from 1.1 to 7
- lambdas: float32 [16], replicated, may hold values from 0.3 to 0.8
- head_gain: float32 [128], replicated, may hold values from 0.1 to 1.9
- out_weight: bfloat16 [2048, 2048], P(None, 'dp'), may hold values from -0.125 to 0.125
Outputs:
- attended: bfloat16 [8, 512, 2048], P(('grp', 'dp'), 'sp'), parts along dimension 0
The draws below stay inside these ranges and needn't reach their ends.
There are 2 independent parts, one for each index of `grp`. The reference program is written for one: setup_inputs(seed, part) draws one part's arguments, and reference() takes and returns one part's arrays. A program takes and returns all parts, laid end to end along the dimension named above; an argument that names none is the same for every part. Nothing has to cross between parts.
All inputs are finite; a program needn't handle non-finite values.
Results may differ from the reference program's by a relative error of at most 0.008.
The reference program's roundings to bfloat16 on the way count: a program that leaves them out, or rounds other values in their place, can miss the bound.
Values may be sent and summed in bfloat16 or wider, within the bound.
A program may use at most 128 MiB of HBM per device.

```python
import jax
import jax.numpy as jnp
from jax import lax

D = 2048
HEADS = 16
HEAD = 64
VDIM = 128
LENGTH = 512
SEQS = 4


def paired_rows(key):
    shape = (SEQS, LENGTH, HEADS * 2 * HEAD)
    key_part = jnp.clip(jax.random.normal(jax.random.fold_in(key, 101), shape, jnp.float32), -6.0, 6.0)
    query_part = jnp.clip(jax.random.normal(jax.random.fold_in(key, 202), shape, jnp.float32), -6.0, 6.0)
    return (query_part, key_part)


def draw_query_rows(key, part):
    return paired_rows(key)[0].astype(jnp.bfloat16)


def draw_key_rows(key, part):
    return paired_rows(key)[1].astype(jnp.bfloat16)


def gain_draw(key):
    return jax.random.uniform(key, (HEAD,), jnp.float32, 1.1, 1.7)


def draw_query_gain(key, part):
    return gain_draw(jax.random.fold_in(key, 31))


def draw_key_gain(key, part):
    return gain_draw(jax.random.fold_in(key, 32))


def shard_levels(key, shape, cuts, smallest, largest):
    level, own = 1.0, jax.random.fold_in(key, 6)
    for dim, shards_of in cuts:
        steps = jnp.exp(jax.random.uniform(jax.random.fold_in(own, dim), (shards_of,), jnp.float32, smallest / len(cuts), largest / len(cuts)))
        level = level * jnp.repeat(steps, shape[dim] // shards_of).reshape([-1 if axis == dim else 1 for axis in range(len(shape))])
    return level


def noise(rng, shape, scale, limit, split=(), kind=jnp.bfloat16):
    factor_of = shard_levels(rng, shape, split, -0.22, 0.18) if split else 1.0
    values = jax.random.normal(rng, shape, jnp.float32) * scale * factor_of
    return jnp.minimum(jnp.maximum(values, -limit), limit).astype(kind)


def setup_inputs(seed: int = 0, part: int = 0) -> dict:
    key_of = jax.random.split(jax.random.key(seed), 9)
    own_keys = jax.random.split(jax.random.fold_in(key_of[8], part), 9)
    query_rows = draw_query_rows(jax.random.fold_in(jax.random.fold_in(key_of[8], part), 71), part)
    key_rows = draw_key_rows(jax.random.fold_in(jax.random.fold_in(key_of[8], part), 71), part)
    value_rows = noise(own_keys[2], (SEQS, LENGTH, HEADS * VDIM), 1.0, 6.0, ((0, 4), (1, 4)))
    query_gain = draw_query_gain(jax.random.fold_in(key_of[8], 71), part)
    key_gain = draw_key_gain(jax.random.fold_in(key_of[8], 71), part)
    lambdas = jnp.clip(jax.random.uniform(key_of[5], (HEADS,), jnp.float32, 0.3, 0.8), 0.3, 0.8)
    head_gain = jnp.clip(1.0 + 0.18 * jax.random.normal(key_of[6], (VDIM,), jnp.float32), 0.1, 1.9)
    out_weight = noise(key_of[7], (HEADS * VDIM, D), (HEADS * VDIM) ** -0.5, 0.125, ((1, 4),))
    return {"query_rows": query_rows, "key_rows": key_rows, "value_rows": value_rows, "query_gain": query_gain, "key_gain": key_gain, "lambdas": lambdas, "head_gain": head_gain, "out_weight": out_weight}


EPSILON = 1e-06
OUT_SCALE = 0.8

def norm_rotate(field_rows, gain_vector, positions):
    widened = field_rows.astype(jnp.float32)
    normed = widened * lax.rsqrt(lax.optimization_barrier(jnp.mean(widened * widened, axis=-1, keepdims=True)) + EPSILON) * gain_vector
    half_size = field_rows.shape[-1] // 2
    inverse = 10000.0 ** (-jnp.arange(half_size, dtype=jnp.float32) / half_size)
    angles = (positions[:, None] * inverse[None, :]).reshape(positions.shape[0], 1, 1, half_size)
    cosine_part = jnp.cos(angles)
    sine_part = jnp.sin(angles)
    first_half = normed[..., :half_size]
    second_half = normed[..., half_size:]
    turned = jnp.concatenate([first_half * cosine_part - second_half * sine_part, second_half * cosine_part + first_half * sine_part], axis=-1)
    return turned.astype(jnp.bfloat16)

def head_norm(raw_heads, gain_vector):
    scaled = raw_heads * lax.rsqrt(lax.optimization_barrier(jnp.mean(raw_heads * raw_heads, axis=-1, keepdims=True)) + EPSILON)
    return (scaled * gain_vector * OUT_SCALE).astype(jnp.bfloat16)

def block_size(length):
    return 512 if length % 512 == 0 else length

def attend(query_head, key_head, value_head, weight_two, gain_vector):
    length = query_head.shape[0]
    block_rows = block_size(length)
    score_scale = query_head.shape[-1] ** (-0.5)
    key_wide = key_head.astype(jnp.float32)
    key_positions = jnp.arange(length, dtype=jnp.int32)

    def one_block(number):
        first_row = number * block_rows
        query_block = lax.dynamic_slice_in_dim(query_head, first_row, block_rows, 0).astype(jnp.float32)
        scores = jnp.einsum('qcd,kcd->cqk', query_block, key_wide) * score_scale
        query_positions = first_row + jnp.arange(block_rows, dtype=jnp.int32)
        visible = key_positions[None, :] <= query_positions[:, None]
        scores = jnp.where(visible[None], scores, -1e+30)
        highest = lax.optimization_barrier(jnp.max(scores, axis=-1, keepdims=True))
        exponent = jnp.exp(scores - highest)
        probabilities = exponent / lax.optimization_barrier(jnp.sum(exponent, axis=-1, keepdims=True))
        mixing = (probabilities[0] - weight_two * probabilities[1]).astype(jnp.bfloat16)
        return jnp.dot(mixing, value_head, preferred_element_type=jnp.float32)
    blocks = lax.map(one_block, jnp.arange(length // block_rows, dtype=jnp.int32))
    return head_norm(blocks.reshape(length, value_head.shape[-1]), gain_vector)

def reference(query_rows, key_rows, value_rows, query_gain, key_gain, lambdas, head_gain, out_weight):
    seq_count = query_rows.shape[0]
    length = query_rows.shape[1]
    positions = jnp.arange(length, dtype=jnp.float32)
    query_rot = norm_rotate(query_rows.reshape(seq_count, length, HEADS, 2, HEAD), query_gain, positions)
    key_rot = norm_rotate(key_rows.reshape(seq_count, length, HEADS, 2, HEAD), key_gain, positions)
    value_heads = value_rows.reshape(seq_count, length, HEADS, VDIM)

    def per_item(number):
        seq_index = number // HEADS
        head_index = number % HEADS
        return attend(query_rot[seq_index, :, head_index], key_rot[seq_index, :, head_index], value_heads[seq_index, :, head_index], lambdas[head_index], head_gain)
    outputs = lax.map(per_item, jnp.arange(seq_count * HEADS, dtype=jnp.int32))
    outputs = outputs.reshape(seq_count, HEADS, length, VDIM).transpose(0, 2, 1, 3)
    outputs = outputs.reshape(seq_count * length, HEADS * VDIM)
    attended = jnp.dot(outputs, out_weight, preferred_element_type=jnp.float32).astype(jnp.bfloat16)
    return attended.reshape(seq_count, length, out_weight.shape[1])
```

```python
import functools
import math

import jax
import jax.numpy as jnp
import numpy as np
from jax import lax
from jax.experimental import pallas as pl
from jax.experimental.pallas import tpu as pltpu
from jax.sharding import PartitionSpec as P

EPSILON = 1e-06
OUT_SCALE = 0.8
CORES = 2
CHUNKS = 2
MESH = pl.DeviceIdType.MESH


def rotation_tables(length, head_size):
    half = head_size // 2
    inverse = np.float32(10000.0) ** (-np.arange(half, dtype=np.float32) / np.float32(half))
    angles = np.arange(length, dtype=np.float32)[:, None] * inverse.astype(np.float32)[None, :]
    cosine, sine = np.cos(angles), np.sin(angles)
    return (
        np.concatenate([cosine] * 4, axis=1).astype(np.float32),
        np.concatenate([-sine, sine] * 2, axis=1).astype(np.float32),
    )


def kernel(
    n, n_dp, head_size, q_ref, k_ref, v_ref, qg_ref, kg_ref, lam_ref, hg_ref, w_ref, cos_ref, sin_ref,
    out_ref, rx, rot_q, rot_k, heads_out, hrx, wfull,
    in_send, in_recv, ret_send, ret_recv, wx_send, wx_recv, wc_send, wc_recv, own_sem,
):
    me = lax.axis_index("sp")
    dp = lax.axis_index("dp")
    cores = CORES if n_dp % CORES == 0 else 1
    nx = n_dp // cores
    xi, core = dp // cores, lax.rem(dp, cores)
    tok = q_ref.shape[1]
    width = 2 * head_size
    local_heads = rx.shape[1]
    length = rx.shape[2]
    depth = w_ref.shape[0]
    cols = w_ref.shape[1]
    piece = depth // CHUNKS

    def sp_peer(off):
        return lax.rem(me + off, n)

    def dp_index(xo, co):
        return lax.rem(xi + xo, nx) * cores + lax.rem(core + co, cores)

    barrier = pltpu.get_barrier_semaphore()
    for off in range(1, n):
        pl.semaphore_signal(barrier, inc=1, device_id={"sp": sp_peer(off)}, device_id_type=MESH)
    for xo in range(1, nx):
        pl.semaphore_signal(barrier, inc=1, device_id={"dp": dp_index(xo, 0)}, device_id_type=MESH)
    for co in range(1, cores):
        pl.semaphore_signal(barrier, inc=1, device_id={"dp": dp_index(0, co)}, device_id_type=MESH)

    sources = (k_ref, q_ref, v_ref)

    def own_rows(t, j):
        column = pl.multiple_of((me * local_heads + j) * width, width)
        return pltpu.make_async_copy(
            sources[t].at[0, :, pl.ds(column, width)],
            rx.at[t, j, pl.ds(pl.multiple_of(me * tok, tok), tok), :],
            in_recv.at[t, j, 0],
        )

    def rows_to(t, j, off):
        peer = sp_peer(off)
        column = pl.multiple_of((peer * local_heads + j) * width, width)
        return pltpu.make_async_remote_copy(
            src_ref=sources[t].at[0, :, pl.ds(column, width)],
            dst_ref=rx.at[t, j, pl.ds(pl.multiple_of(me * tok, tok), tok), :],
            send_sem=in_send.at[t, j, off],
            recv_sem=in_recv.at[t, j, off],
            device_id={"sp": peer},
            device_id_type=MESH,
        )

    def rows_from(t, j, off):
        peer = lax.rem(me + n - off, n)
        block = rx.at[t, j, pl.ds(pl.multiple_of(peer * tok, tok), tok), :]
        return pltpu.make_async_remote_copy(
            src_ref=block, dst_ref=block, send_sem=in_send.at[t, j, off],
            recv_sem=in_recv.at[t, j, off], device_id={"sp": peer}, device_id_type=MESH,
        )

    def weight_x(xo, r):
        rows = pl.ds(r * piece, piece)
        return pltpu.make_async_remote_copy(
            src_ref=w_ref.at[rows, :], dst_ref=wfull.at[dp, rows, :],
            send_sem=wx_send.at[xo, r], recv_sem=wx_recv.at[xo, r],
            device_id={"dp": dp_index(xo, 0)}, device_id_type=MESH,
        )

    def weight_x_in(xo, r):
        block = wfull.at[dp_index(nx - xo, 0), pl.ds(r * piece, piece), :]
        return pltpu.make_async_remote_copy(
            src_ref=block, dst_ref=block, send_sem=wx_send.at[xo, r], recv_sem=wx_recv.at[xo, r],
            device_id={"dp": dp_index(xo, 0)}, device_id_type=MESH,
        )

    def weight_core(xo, r):
        rows = pl.ds(r * piece, piece)
        target = wfull.at[dp_index(nx - xo, 0), rows, :]
        return pltpu.make_async_remote_copy(
            src_ref=w_ref.at[rows, :] if xo == 0 else target, dst_ref=target,
            send_sem=wc_send.at[xo, r], recv_sem=wc_recv.at[xo, r],
            device_id={"dp": dp_index(0, 1)}, device_id_type=MESH,
        )

    def weight_core_in(xo, r):
        block = wfull.at[dp_index(nx - xo, 1), pl.ds(r * piece, piece), :]
        return pltpu.make_async_remote_copy(
            src_ref=block, dst_ref=block, send_sem=wc_send.at[xo, r], recv_sem=wc_recv.at[xo, r],
            device_id={"dp": dp_index(0, 1)}, device_id_type=MESH,
        )

    own_weight = pltpu.make_async_copy(w_ref, wfull.at[dp], own_sem)
    own_weight.start()
    for j in range(local_heads):
        for t in range(3):
            own_rows(t, j).start()
    pl.semaphore_wait(barrier, (n - 1) + (nx - 1) + (cores - 1))
    for j in range(local_heads):
        for t in range(3):
            for off in range(1, n):
                rows_to(t, j, off).start()
        if j == 0:
            for r in range(CHUNKS):
                for xo in range(1, nx):
                    weight_x(xo, r).start()
            if cores > 1:
                for r in range(CHUNKS):
                    weight_core(0, r).start()

    lane = lax.broadcasted_iota(jnp.int32, (1, width), 1)
    low_map = lane < head_size
    low_half = lax.rem(lane, head_size) < head_size // 2

    def norm_rotate(block, gain):
        x = block.astype(jnp.float32)
        square = x * x
        low = jnp.sum(jnp.where(low_map, square, 0.0), axis=1, keepdims=True)
        high = jnp.sum(jnp.where(low_map, 0.0, square), axis=1, keepdims=True)
        low = lax.rsqrt(low * (1.0 / head_size) + EPSILON)
        high = lax.rsqrt(high * (1.0 / head_size) + EPSILON)
        y = x * jnp.where(low_map, low, high) * gain
        quarter = head_size // 2
        turned = jnp.where(low_half, pltpu.roll(y, width - quarter, 1), pltpu.roll(y, quarter, 1))
        return (y * cos_ref[...] + turned * sin_ref[...]).astype(jnp.bfloat16)

    def heads_to(j, i):
        column = pl.multiple_of((me * local_heads + j) * width, width)
        off = lax.rem(i + n - me, n)
        return pltpu.make_async_remote_copy(
            src_ref=heads_out.at[j, i], dst_ref=hrx.at[:, pl.ds(column, width)],
            send_sem=ret_send.at[j, off], recv_sem=ret_recv.at[j, off],
            device_id={"sp": i}, device_id_type=MESH,
        )

    def heads_from(j, off):
        peer = lax.rem(me + n - off, n)
        column = pl.multiple_of((peer * local_heads + j) * width, width)
        block = hrx.at[:, pl.ds(column, width)]
        return pltpu.make_async_remote_copy(
            src_ref=block, dst_ref=block, send_sem=ret_send.at[j, off],
            recv_sem=ret_recv.at[j, off], device_id={"sp": peer}, device_id_type=MESH,
        )

    groups = math.gcd(n, 4)
    per_group = n // groups
    segment = length // groups
    factor = head_size ** (-0.5) * math.log2(math.e)
    contract = (((1,), (1,)), ((), ()))

    def query_block(j, g, i, lam):
        rows = pl.ds(i * tok, tok) if isinstance(i, int) else pl.ds(pl.multiple_of(i * tok, tok), tok)
        q = rot_q[rows, :]
        zero = jnp.zeros_like(q)
        both = jnp.concatenate([jnp.where(low_map, q, zero), jnp.where(low_map, zero, q)], axis=0)
        start = g * segment
        spans = ([(0, start)] if g else []) + [(start, segment)]
        parts = []
        for first, size in spans:
            scores = lax.dot_general(
                both, rot_k[first : first + size, :], contract, preferred_element_type=jnp.float32
            )
            if first == start:
                shape = (2 * tok, size)
                row = lax.rem(lax.broadcasted_iota(jnp.int32, shape, 0), tok) + i * tok
                column = lax.broadcasted_iota(jnp.int32, shape, 1) + first
                scores = jnp.where(column <= row, scores, -1e30)
            parts.append(scores)
        top = functools.reduce(jnp.maximum, [jnp.max(s, axis=1, keepdims=True) for s in parts])
        parts = [jnp.exp2((s - top) * factor) for s in parts]
        total = functools.reduce(jnp.add, [jnp.sum(e, axis=1, keepdims=True) for e in parts])
        inverse = 1.0 / total
        one, two = inverse[:tok], inverse[tok:] * lam
        raw = None
        for (first, size), e in zip(spans, parts):
            mixing = (e[:tok] * one - e[tok:] * two).astype(jnp.bfloat16)
            term = jnp.dot(mixing, rx[2, j, first : first + size, :], preferred_element_type=jnp.float32)
            raw = term if raw is None else raw + term
        scaled = raw * lax.rsqrt(jnp.mean(raw * raw, axis=1, keepdims=True) + EPSILON)
        result = (scaled * hg_ref[...] * OUT_SCALE).astype(jnp.bfloat16)

        @pl.when(i == me)
        def _():
            column = pl.multiple_of((me * local_heads + j) * width, width)
            hrx[:, pl.ds(column, width)] = result

        @pl.when(i != me)
        def _():
            heads_out[j, i] = result
            heads_to(j, i).start()

    def forward(r):
        if cores > 1:
            for xo in range(1, nx):
                weight_x_in(xo, r).wait_recv()
                weight_core(xo, r).start()

    for j in range(local_heads):
        lam = lam_ref[me * local_heads + j]
        for t, (target, gain) in enumerate(((rot_k, kg_ref), (rot_q, qg_ref), (None, None))):
            own_rows(t, j).wait()
            for off in range(1, n):
                rows_from(t, j, off).wait_recv()
            if target is not None:
                target[...] = norm_rotate(rx[t, j], gain[...])
        for g in range(groups):
            if per_group == 1:
                query_block(j, g, g, lam)
            else:
                def step(b, carry, j=j, g=g, lam=lam):
                    query_block(j, g, g * per_group + b, lam)
                    return carry
                lax.fori_loop(0, per_group, step, 0)
        if j == max(local_heads - 2, 0):
            forward(0)
    for r in range(1, CHUNKS):
        forward(r)

    for j in range(local_heads):
        for off in range(1, n):
            heads_from(j, off).wait_recv()
    own_weight.wait()
    rows = hrx[...]

    def project(index):
        column = pl.multiple_of(index * cols, cols)
        out_ref[0, :, pl.ds(column, cols)] = jnp.dot(
            rows, wfull[index], preferred_element_type=jnp.float32
        ).astype(out_ref.dtype)

    for co in range(cores):
        for xo in range(nx):
            for r in range(CHUNKS):
                if co:
                    weight_core_in(xo, r).wait_recv()
                elif xo and cores == 1:
                    weight_x_in(xo, r).wait_recv()
            project(dp_index(nx - xo, co))

    for j in range(local_heads):
        for off in range(1, n):
            for t in range(3):
                rows_to(t, j, off).wait_send()
            heads_to(j, sp_peer(off)).wait_send()
    for r in range(CHUNKS):
        for xo in range(nx):
            if xo:
                weight_x(xo, r).wait_send()
            if cores > 1:
                weight_core(xo, r).wait_send()


def local(n, n_dp, query_rows, key_rows, value_rows, query_gain, key_gain, lambdas, head_gain, out_weight):
    tok = query_rows.shape[1]
    head_size = query_gain.shape[0]
    width = head_gain.shape[0]
    local_heads = lambdas.shape[0] // n
    length = tok * n
    depth, cols = out_weight.shape
    cores = CORES if n_dp % CORES == 0 else 1
    nx = n_dp // cores
    cosine, sine = rotation_tables(length, head_size)
    anywhere = pl.BlockSpec(memory_space=pl.ANY)
    vmem = pl.BlockSpec(memory_space=pltpu.VMEM)
    dma = pltpu.SemaphoreType.DMA
    return pl.pallas_call(
        functools.partial(kernel, n, n_dp, head_size),
        out_shape=jax.ShapeDtypeStruct((1, tok, n_dp * cols), jnp.bfloat16),
        in_specs=[anywhere] * 3
        + [vmem, vmem, pl.BlockSpec(memory_space=pltpu.SMEM), vmem, anywhere, vmem, vmem],
        out_specs=vmem,
        scratch_shapes=[
            pltpu.VMEM((3, local_heads, length, width), jnp.bfloat16),
            pltpu.VMEM((length, width), jnp.bfloat16),
            pltpu.VMEM((length, width), jnp.bfloat16),
            pltpu.VMEM((local_heads, n, tok, width), jnp.bfloat16),
            pltpu.VMEM((tok, depth), jnp.bfloat16),
            pltpu.VMEM((n_dp, depth, cols), jnp.bfloat16),
            dma((3, local_heads, n)),
            dma((3, local_heads, n)),
            dma((local_heads, n)),
            dma((local_heads, n)),
            dma((nx, CHUNKS)),
            dma((nx, CHUNKS)),
            dma((nx, CHUNKS)),
            dma((nx, CHUNKS)),
            dma(()),
        ],
        compiler_params=pltpu.CompilerParams(
            collective_id=0, has_side_effects=True, vmem_limit_bytes=56 * 1024 * 1024
        ),
    )(
        query_rows, key_rows, value_rows,
        jnp.tile(query_gain, 2)[None, :], jnp.tile(key_gain, 2)[None, :], lambdas, head_gain[None, :],
        out_weight, jnp.asarray(cosine), jnp.asarray(sine),
    )


def solution(mesh):
    rows = P(("grp", "dp"), "sp", None)
    return jax.shard_map(
        functools.partial(local, mesh.shape["sp"], mesh.shape["dp"]),
        mesh=mesh,
        in_specs=(rows, rows, rows, P(), P(), P(), P(), P(None, "dp")),
        out_specs=rows,
        check_vma=False,
    )
```

```python
import functools
import math

import jax
import jax.numpy as jnp
import numpy as np
from jax import lax
from jax.experimental import pallas as pl
from jax.experimental.pallas import tpu as pltpu
from jax.sharding import PartitionSpec as P

EPSILON = 1e-06
OUT_SCALE = 0.8
CORES = 2
CHUNKS = 2
WAYS = 2
MESH = pl.DeviceIdType.MESH


def rotation_tables(length, head_size):
    half = head_size // 2
    inverse = np.float32(10000.0) ** (-np.arange(half, dtype=np.float32) / np.float32(half))
    angles = np.arange(length, dtype=np.float32)[:, None] * inverse.astype(np.float32)[None, :]
    cosine, sine = np.cos(angles), np.sin(angles)
    return (
        np.concatenate([cosine] * 4, axis=1).astype(np.float32),
        np.concatenate([-sine, sine] * 2, axis=1).astype(np.float32),
    )


def kernel(
    n, n_dp, n_grp, head_size, q_ref, k_ref, v_ref, qg_ref, kg_ref, lam_ref, hg_ref, w_ref, cos_ref, sin_ref,
    out_ref, total, rx, rot_q, rot_k, heads_out, hrx, wfull,
    in_send, in_recv, ret_send, ret_recv, wx_send, wx_recv, wy_send, wy_recv, wc_send, wc_recv, own_sem,
):
    me = lax.axis_index("sp")
    dp = lax.axis_index("dp")
    ways = WAYS if n_grp == WAYS else 1
    grp = lax.axis_index("grp") if ways > 1 else 0
    cores = CORES if n_dp % CORES == 0 else 1
    nx = n_dp // cores
    xi, core = dp // cores, lax.rem(dp, cores)
    tok = q_ref.shape[1]
    width = 2 * head_size
    local_heads = rx.shape[1]
    length = rx.shape[2]
    depth = w_ref.shape[0]
    cols = w_ref.shape[1]
    piece = depth // (CHUNKS * ways)

    def sp_peer(off):
        return lax.rem(me + off, n)

    def dp_index(xo, co):
        return lax.rem(xi + xo, nx) * cores + lax.rem(core + co, cores)

    barrier = pltpu.get_barrier_semaphore()
    for off in range(1, n):
        pl.semaphore_signal(barrier, inc=1, device_id={"sp": sp_peer(off)}, device_id_type=MESH)
    for xo in range(1, nx):
        pl.semaphore_signal(barrier, inc=1, device_id={"dp": dp_index(xo, 0)}, device_id_type=MESH)
    for co in range(1, cores):
        pl.semaphore_signal(barrier, inc=1, device_id={"dp": dp_index(0, co)}, device_id_type=MESH)

    if ways > 1:
        pl.semaphore_signal(
            barrier, inc=1, device_id={"grp": lax.rem(grp + 1, ways)}, device_id_type=MESH
        )

    sources = (k_ref, q_ref, v_ref)

    def own_rows(t, j):
        column = pl.multiple_of((me * local_heads + j) * width, width)
        return pltpu.make_async_copy(
            sources[t].at[0, :, pl.ds(column, width)],
            rx.at[t, j, pl.ds(pl.multiple_of(me * tok, tok), tok), :],
            in_recv.at[t, j, 0],
        )

    def rows_to(t, j, off):
        peer = sp_peer(off)
        column = pl.multiple_of((peer * local_heads + j) * width, width)
        return pltpu.make_async_remote_copy(
            src_ref=sources[t].at[0, :, pl.ds(column, width)],
            dst_ref=rx.at[t, j, pl.ds(pl.multiple_of(me * tok, tok), tok), :],
            send_sem=in_send.at[t, j, off],
            recv_sem=in_recv.at[t, j, off],
            device_id={"sp": peer},
            device_id_type=MESH,
        )

    def rows_from(t, j, off):
        peer = lax.rem(me + n - off, n)
        block = rx.at[t, j, pl.ds(pl.multiple_of(peer * tok, tok), tok), :]
        return pltpu.make_async_remote_copy(
            src_ref=block, dst_ref=block, send_sem=in_send.at[t, j, off],
            recv_sem=in_recv.at[t, j, off], device_id={"sp": peer}, device_id_type=MESH,
        )

    def piece_rows(r, way):
        first = (r * ways + lax.rem(grp + way, ways)) * piece
        return pl.ds(pl.multiple_of(first, piece), piece)

    def moved(source, target, send_sem, recv_sem, device):
        return pltpu.make_async_remote_copy(
            src_ref=source, dst_ref=target, send_sem=send_sem, recv_sem=recv_sem,
            device_id=device, device_id_type=MESH,
        )

    def weight_x(xo, r):
        rows = piece_rows(r, 0)
        return moved(
            w_ref.at[rows, :], wfull.at[dp, rows, :], wx_send.at[xo, r], wx_recv.at[xo, r],
            {"dp": dp_index(xo, 0)},
        )

    def weight_x_in(xo, r):
        block = wfull.at[dp_index(nx - xo, 0), piece_rows(r, 0), :]
        return moved(block, block, wx_send.at[xo, r], wx_recv.at[xo, r], {"dp": dp_index(xo, 0)})

    def weight_y(xo, r):
        block = wfull.at[dp_index(nx - xo, 0), piece_rows(r, 0), :]
        return moved(block, block, wy_send.at[xo, r], wy_recv.at[xo, r], {"grp": lax.rem(grp + 1, ways)})

    def weight_y_in(xo, r):
        block = wfull.at[dp_index(nx - xo, 0), piece_rows(r, 1), :]
        return moved(block, block, wy_send.at[xo, r], wy_recv.at[xo, r], {"grp": lax.rem(grp + 1, ways)})

    def weight_core(xo, r, way):
        rows = piece_rows(r, way)
        target = wfull.at[dp_index(nx - xo, 0), rows, :]
        return moved(
            w_ref.at[rows, :] if xo == 0 else target, target,
            wc_send.at[xo, r, way], wc_recv.at[xo, r, way], {"dp": dp_index(0, 1)},
        )

    def weight_core_in(xo, r, way):
        block = wfull.at[dp_index(nx - xo, 1), piece_rows(r, way), :]
        return moved(
            block, block, wc_send.at[xo, r, way], wc_recv.at[xo, r, way], {"dp": dp_index(0, 1)}
        )

    own_weight = pltpu.make_async_copy(w_ref, wfull.at[dp], own_sem)
    own_weight.start()
    for j in range(local_heads):
        for t in range(3):
            own_rows(t, j).start()
    pl.semaphore_wait(barrier, (n - 1) + (nx - 1) + (cores - 1) + (ways - 1))
    for j in range(local_heads):
        for t in range(3):
            for off in range(1, n):
                rows_to(t, j, off).start()
        if j == 0:
            for r in range(CHUNKS):
                for xo in range(1, nx):
                    weight_x(xo, r).start()
            if cores > 1:
                for r in range(CHUNKS):
                    for way in range(ways):
                        weight_core(0, r, way).start()

    lane = lax.broadcasted_iota(jnp.int32, (1, width), 1)
    low_map = lane < head_size
    low_half = lax.rem(lane, head_size) < head_size // 2

    def norm_rotate(block, gain):
        x = block.astype(jnp.float32)
        square = x * x
        low = jnp.sum(jnp.where(low_map, square, 0.0), axis=1, keepdims=True)
        high = jnp.sum(jnp.where(low_map, 0.0, square), axis=1, keepdims=True)
        low = lax.rsqrt(low * (1.0 / head_size) + EPSILON)
        high = lax.rsqrt(high * (1.0 / head_size) + EPSILON)
        y = x * jnp.where(low_map, low, high) * gain
        quarter = head_size // 2
        turned = jnp.where(low_half, pltpu.roll(y, width - quarter, 1), pltpu.roll(y, quarter, 1))
        return (y * cos_ref[...] + turned * sin_ref[...]).astype(jnp.bfloat16)

    def heads_to(j, i):
        column = pl.multiple_of(me * width, width)
        off = lax.rem(i + n - me, n)
        return pltpu.make_async_remote_copy(
            src_ref=heads_out.at[j, i], dst_ref=hrx.at[j, :, pl.ds(column, width)],
            send_sem=ret_send.at[j, off], recv_sem=ret_recv.at[j, off],
            device_id={"sp": i}, device_id_type=MESH,
        )

    def heads_from(j, off):
        peer = lax.rem(me + n - off, n)
        column = pl.multiple_of(peer * width, width)
        block = hrx.at[j, :, pl.ds(column, width)]
        return pltpu.make_async_remote_copy(
            src_ref=block, dst_ref=block, send_sem=ret_send.at[j, off],
            recv_sem=ret_recv.at[j, off], device_id={"sp": peer}, device_id_type=MESH,
        )

    groups = math.gcd(n, 4)
    per_group = n // groups
    segment = length // groups
    factor = head_size ** (-0.5) * math.log2(math.e)
    contract = (((1,), (1,)), ((), ()))

    def query_block(j, g, i, lam):
        rows = pl.ds(i * tok, tok) if isinstance(i, int) else pl.ds(pl.multiple_of(i * tok, tok), tok)
        q = rot_q[rows, :]
        zero = jnp.zeros_like(q)
        both = jnp.concatenate([jnp.where(low_map, q, zero), jnp.where(low_map, zero, q)], axis=0)
        start = g * segment
        spans = ([(0, start)] if g else []) + [(start, segment)]
        parts = []
        for first, size in spans:
            scores = lax.dot_general(
                both, rot_k[first : first + size, :], contract, preferred_element_type=jnp.float32
            )
            if first == start:
                shape = (2 * tok, size)
                row = lax.rem(lax.broadcasted_iota(jnp.int32, shape, 0), tok) + i * tok
                column = lax.broadcasted_iota(jnp.int32, shape, 1) + first
                scores = jnp.where(column <= row, scores, -1e30)
            parts.append(scores)
        top = functools.reduce(jnp.maximum, [jnp.max(s, axis=1, keepdims=True) for s in parts])
        parts = [jnp.exp2((s - top) * factor) for s in parts]
        total = functools.reduce(jnp.add, [jnp.sum(e, axis=1, keepdims=True) for e in parts])
        inverse = 1.0 / total
        one, two = inverse[:tok], inverse[tok:] * lam
        raw = None
        for (first, size), e in zip(spans, parts):
            mixing = (e[:tok] * one - e[tok:] * two).astype(jnp.bfloat16)
            term = jnp.dot(mixing, rx[2, j, first : first + size, :], preferred_element_type=jnp.float32)
            raw = term if raw is None else raw + term
        scaled = raw * lax.rsqrt(jnp.mean(raw * raw, axis=1, keepdims=True) + EPSILON)
        result = (scaled * hg_ref[...] * OUT_SCALE).astype(jnp.bfloat16)

        @pl.when(i == me)
        def _():
            hrx[j, :, pl.ds(pl.multiple_of(me * width, width), width)] = result

        @pl.when(i != me)
        def _():
            heads_out[j, i] = result
            heads_to(j, i).start()

    def forward(stage):
        if stage < CHUNKS:
            for xo in range(1, nx):
                weight_x_in(xo, stage).wait_recv()
                if ways > 1:
                    weight_y(xo, stage).start()
                if cores > 1:
                    weight_core(xo, stage, 0).start()
        elif ways > 1:
            for xo in range(1, nx):
                weight_y_in(xo, stage - CHUNKS).wait_recv()
                if cores > 1:
                    weight_core(xo, stage - CHUNKS, 1).start()

    for j in range(local_heads):
        lam = lam_ref[me * local_heads + j]
        for t, (target, gain) in enumerate(((rot_k, kg_ref), (rot_q, qg_ref), (None, None))):
            own_rows(t, j).wait()
            for off in range(1, n):
                rows_from(t, j, off).wait_recv()
            if target is not None:
                target[...] = norm_rotate(rx[t, j], gain[...])
        for g in range(groups):
            if per_group == 1:
                query_block(j, g, g, lam)
            else:
                def step(b, carry, j=j, g=g, lam=lam):
                    query_block(j, g, g * per_group + b, lam)
                    return carry
                lax.fori_loop(0, per_group, step, 0)
        for stage in range(2 * CHUNKS):
            if j == min(stage, local_heads - 1):
                forward(stage)

    own_weight.wait()
    if cores > 1:
        for xo in range(nx):
            for r in range(CHUNKS):
                for way in range(ways):
                    weight_core_in(xo, r, way).wait_recv()

    for j in range(local_heads):
        for off in range(1, n):
            heads_from(j, off).wait_recv()
        rows = hrx[j]
        for index in range(n_dp):
            matching = jnp.concatenate(
                [wfull[index, pl.ds((s * local_heads + j) * width, width), :] for s in range(n)], axis=0
            )
            term = jnp.dot(rows, matching, preferred_element_type=jnp.float32)
            span = slice(index * cols, (index + 1) * cols)
            if j:
                term = total[:, span] + term
            if j == local_heads - 1:
                out_ref[0, :, span] = term.astype(out_ref.dtype)
            else:
                total[:, span] = term

    for j in range(local_heads):
        for off in range(1, n):
            for t in range(3):
                rows_to(t, j, off).wait_send()
            heads_to(j, sp_peer(off)).wait_send()
    for r in range(CHUNKS):
        for xo in range(nx):
            if xo:
                weight_x(xo, r).wait_send()
                if ways > 1:
                    weight_y(xo, r).wait_send()
            if cores > 1:
                for way in range(ways):
                    weight_core(xo, r, way).wait_send()


def local(n, n_dp, n_grp, query_rows, key_rows, value_rows, query_gain, key_gain, lambdas, head_gain, out_weight):
    tok = query_rows.shape[1]
    head_size = query_gain.shape[0]
    width = head_gain.shape[0]
    local_heads = lambdas.shape[0] // n
    length = tok * n
    depth, cols = out_weight.shape
    cores = CORES if n_dp % CORES == 0 else 1
    nx = n_dp // cores
    cosine, sine = rotation_tables(length, head_size)
    anywhere = pl.BlockSpec(memory_space=pl.ANY)
    vmem = pl.BlockSpec(memory_space=pltpu.VMEM)
    dma = pltpu.SemaphoreType.DMA
    return pl.pallas_call(
        functools.partial(kernel, n, n_dp, n_grp, head_size),
        out_shape=jax.ShapeDtypeStruct((1, tok, n_dp * cols), jnp.bfloat16),
        in_specs=[anywhere] * 3
        + [vmem, vmem, pl.BlockSpec(memory_space=pltpu.SMEM), vmem, anywhere, vmem, vmem],
        out_specs=vmem,
        scratch_shapes=[
            pltpu.VMEM((tok, n_dp * cols), jnp.float32),
            pltpu.VMEM((3, local_heads, length, width), jnp.bfloat16),
            pltpu.VMEM((length, width), jnp.bfloat16),
            pltpu.VMEM((length, width), jnp.bfloat16),
            pltpu.VMEM((local_heads, n, tok, width), jnp.bfloat16),
            pltpu.VMEM((local_heads, tok, n * width), jnp.bfloat16),
            pltpu.VMEM((n_dp, depth, cols), jnp.bfloat16),
            dma((3, local_heads, n)),
            dma((3, local_heads, n)),
            dma((local_heads, n)),
            dma((local_heads, n)),
            dma((nx, CHUNKS)),
            dma((nx, CHUNKS)),
            dma((nx, CHUNKS)),
            dma((nx, CHUNKS)),
            dma((nx, CHUNKS, WAYS)),
            dma((nx, CHUNKS, WAYS)),
            dma(()),
        ],
        compiler_params=pltpu.CompilerParams(
            collective_id=0, has_side_effects=True, vmem_limit_bytes=56 * 1024 * 1024
        ),
    )(
        query_rows, key_rows, value_rows,
        jnp.tile(query_gain, 2)[None, :], jnp.tile(key_gain, 2)[None, :], lambdas, head_gain[None, :],
        out_weight, jnp.asarray(cosine), jnp.asarray(sine),
    )


def solution(mesh):
    rows = P(("grp", "dp"), "sp", None)
    return jax.shard_map(
        functools.partial(local, mesh.shape["sp"], mesh.shape["dp"], mesh.shape["grp"]),
        mesh=mesh,
        in_specs=(rows, rows, rows, P(), P(), P(), P(), P(None, "dp")),
        out_specs=rows,
        check_vma=False,
    )
```

```python
import functools
import math

import jax
import jax.numpy as jnp
import numpy as np
from jax import lax
from jax.experimental import pallas as pl
from jax.experimental.pallas import tpu as pltpu
from jax.sharding import PartitionSpec as P

EPSILON = 1e-06
OUT_SCALE = 0.8
CORES = 2
CHUNKS = 2
WAYS = 2
MESH = pl.DeviceIdType.MESH


def rotation_tables(length, head_size):
    half = head_size // 2
    inverse = np.float32(10000.0) ** (-np.arange(half, dtype=np.float32) / np.float32(half))
    angles = np.arange(length, dtype=np.float32)[:, None] * inverse.astype(np.float32)[None, :]
    cosine, sine = np.cos(angles), np.sin(angles)
    return (
        np.concatenate([cosine] * 4, axis=1).astype(np.float32),
        np.concatenate([-sine, sine] * 2, axis=1).astype(np.float32),
    )


def kernel(
    n, n_dp, n_grp, head_size, q_ref, k_ref, v_ref, qg_ref, kg_ref, lam_ref, hg_ref, w_ref, cos_in, sin_in,
    out_ref, total, rx, rot_q, rot_k, heads_out, hrx, wfull,
    in_send, in_recv, ret_send, ret_recv, wx_send, wx_recv, wy_send, wy_recv, wc_send, wc_recv, own_sem, cos_ref, sin_ref, table_sem,
):
    me = lax.axis_index("sp")
    dp = lax.axis_index("dp")
    ways = WAYS if n_grp == WAYS else 1
    grp = lax.axis_index("grp") if ways > 1 else 0
    cores = CORES if n_dp % CORES == 0 else 1
    nx = n_dp // cores
    xi, core = dp // cores, lax.rem(dp, cores)
    tok = q_ref.shape[1]
    width = 2 * head_size
    local_heads = rx.shape[1]
    length = rx.shape[2]
    depth = w_ref.shape[0]
    cols = w_ref.shape[1]
    piece = depth // (CHUNKS * ways)

    def sp_peer(off):
        return lax.rem(me + off, n)

    def dp_index(xo, co):
        return lax.rem(xi + xo, nx) * cores + lax.rem(core + co, cores)

    barrier = pltpu.get_barrier_semaphore()
    for off in range(1, n):
        pl.semaphore_signal(barrier, inc=1, device_id={"sp": sp_peer(off)}, device_id_type=MESH)
    for xo in range(1, nx):
        pl.semaphore_signal(barrier, inc=1, device_id={"dp": dp_index(xo, 0)}, device_id_type=MESH)
    for co in range(1, cores):
        pl.semaphore_signal(barrier, inc=1, device_id={"dp": dp_index(0, co)}, device_id_type=MESH)

    if ways > 1:
        pl.semaphore_signal(
            barrier, inc=1, device_id={"grp": lax.rem(grp + 1, ways)}, device_id_type=MESH
        )

    sources = (k_ref, q_ref, v_ref)

    def own_rows(t, j):
        column = pl.multiple_of((me * local_heads + j) * width, width)
        return pltpu.make_async_copy(
            sources[t].at[0, :, pl.ds(column, width)],
            rx.at[t, j, pl.ds(pl.multiple_of(me * tok, tok), tok), :],
            in_recv.at[t, j, 0],
        )

    def rows_to(t, j, off):
        peer = sp_peer(off)
        column = pl.multiple_of((peer * local_heads + j) * width, width)
        return pltpu.make_async_remote_copy(
            src_ref=sources[t].at[0, :, pl.ds(column, width)],
            dst_ref=rx.at[t, j, pl.ds(pl.multiple_of(me * tok, tok), tok), :],
            send_sem=in_send.at[t, j, off],
            recv_sem=in_recv.at[t, j, off],
            device_id={"sp": peer},
            device_id_type=MESH,
        )

    def rows_from(t, j, off):
        peer = lax.rem(me + n - off, n)
        block = rx.at[t, j, pl.ds(pl.multiple_of(peer * tok, tok), tok), :]
        return pltpu.make_async_remote_copy(
            src_ref=block, dst_ref=block, send_sem=in_send.at[t, j, off],
            recv_sem=in_recv.at[t, j, off], device_id={"sp": peer}, device_id_type=MESH,
        )

    def piece_rows(r, way):
        first = (r * ways + lax.rem(grp + way, ways)) * piece
        return pl.ds(pl.multiple_of(first, piece), piece)

    def moved(source, target, send_sem, recv_sem, device):
        return pltpu.make_async_remote_copy(
            src_ref=source, dst_ref=target, send_sem=send_sem, recv_sem=recv_sem,
            device_id=device, device_id_type=MESH,
        )

    def weight_x(xo, r):
        rows = piece_rows(r, 0)
        return moved(
            w_ref.at[rows, :], wfull.at[dp, rows, :], wx_send.at[xo, r], wx_recv.at[xo, r],
            {"dp": dp_index(xo, 0)},
        )

    def weight_x_in(xo, r):
        block = wfull.at[dp_index(nx - xo, 0), piece_rows(r, 0), :]
        return moved(block, block, wx_send.at[xo, r], wx_recv.at[xo, r], {"dp": dp_index(xo, 0)})

    def weight_y(xo, r):
        block = wfull.at[dp_index(nx - xo, 0), piece_rows(r, 0), :]
        return moved(block, block, wy_send.at[xo, r], wy_recv.at[xo, r], {"grp": lax.rem(grp + 1, ways)})

    def weight_y_in(xo, r):
        block = wfull.at[dp_index(nx - xo, 0), piece_rows(r, 1), :]
        return moved(block, block, wy_send.at[xo, r], wy_recv.at[xo, r], {"grp": lax.rem(grp + 1, ways)})

    def weight_core(xo, r, way):
        rows = piece_rows(r, way)
        target = wfull.at[dp_index(nx - xo, 0), rows, :]
        return moved(
            w_ref.at[rows, :] if xo == 0 else target, target,
            wc_send.at[xo, r, way], wc_recv.at[xo, r, way], {"dp": dp_index(0, 1)},
        )

    def weight_core_in(xo, r, way):
        block = wfull.at[dp_index(nx - xo, 1), piece_rows(r, way), :]
        return moved(
            block, block, wc_send.at[xo, r, way], wc_recv.at[xo, r, way], {"dp": dp_index(0, 1)}
        )

    own_weight = pltpu.make_async_copy(w_ref, wfull.at[dp], own_sem)
    own_weight.start()
    tables = [
        pltpu.make_async_copy(cos_in, cos_ref, table_sem.at[0]),
        pltpu.make_async_copy(sin_in, sin_ref, table_sem.at[1]),
    ]
    for table in tables:
        table.start()
    for j in range(local_heads):
        for t in range(3):
            own_rows(t, j).start()
    pl.semaphore_wait(barrier, (n - 1) + (nx - 1) + (cores - 1) + (ways - 1))
    for j in range(local_heads):
        for t in range(3):
            for off in range(1, n):
                rows_to(t, j, off).start()
        if j == 0:
            for r in range(CHUNKS):
                for xo in range(1, nx):
                    weight_x(xo, r).start()
            if cores > 1:
                for r in range(CHUNKS):
                    for way in range(ways):
                        weight_core(0, r, way).start()

    lane = lax.broadcasted_iota(jnp.int32, (1, width), 1)
    low_map = lane < head_size
    low_half = lax.rem(lane, head_size) < head_size // 2

    def norm_rotate(block, gain):
        x = block.astype(jnp.float32)
        square = x * x
        low = jnp.sum(jnp.where(low_map, square, 0.0), axis=1, keepdims=True)
        high = jnp.sum(jnp.where(low_map, 0.0, square), axis=1, keepdims=True)
        low = lax.rsqrt(low * (1.0 / head_size) + EPSILON)
        high = lax.rsqrt(high * (1.0 / head_size) + EPSILON)
        y = x * jnp.where(low_map, low, high) * gain
        quarter = head_size // 2
        turned = jnp.where(low_half, pltpu.roll(y, width - quarter, 1), pltpu.roll(y, quarter, 1))
        return (y * cos_ref[...] + turned * sin_ref[...]).astype(jnp.bfloat16)

    def heads_to(j, i):
        column = pl.multiple_of(me * width, width)
        off = lax.rem(i + n - me, n)
        return pltpu.make_async_remote_copy(
            src_ref=heads_out.at[j, i], dst_ref=hrx.at[j, :, pl.ds(column, width)],
            send_sem=ret_send.at[j, off], recv_sem=ret_recv.at[j, off],
            device_id={"sp": i}, device_id_type=MESH,
        )

    def heads_from(j, off):
        peer = lax.rem(me + n - off, n)
        column = pl.multiple_of(peer * width, width)
        block = hrx.at[j, :, pl.ds(column, width)]
        return pltpu.make_async_remote_copy(
            src_ref=block, dst_ref=block, send_sem=ret_send.at[j, off],
            recv_sem=ret_recv.at[j, off], device_id={"sp": peer}, device_id_type=MESH,
        )

    groups = math.gcd(n, 4)
    per_group = n // groups
    segment = length // groups
    factor = head_size ** (-0.5) * math.log2(math.e)
    contract = (((1,), (1,)), ((), ()))

    def query_block(j, g, i, lam):
        rows = pl.ds(i * tok, tok) if isinstance(i, int) else pl.ds(pl.multiple_of(i * tok, tok), tok)
        q = rot_q[rows, :]
        zero = jnp.zeros_like(q)
        both = jnp.concatenate([jnp.where(low_map, q, zero), jnp.where(low_map, zero, q)], axis=0)
        start = g * segment
        spans = ([(0, start)] if g else []) + [(start, segment)]
        parts = []
        for first, size in spans:
            scores = lax.dot_general(
                both, rot_k[first : first + size, :], contract, preferred_element_type=jnp.float32
            )
            if first == start:
                shape = (2 * tok, size)
                row = lax.rem(lax.broadcasted_iota(jnp.int32, shape, 0), tok) + i * tok
                column = lax.broadcasted_iota(jnp.int32, shape, 1) + first
                scores = jnp.where(column <= row, scores, -1e30)
            parts.append(scores)
        top = functools.reduce(jnp.maximum, [jnp.max(s, axis=1, keepdims=True) for s in parts])
        parts = [jnp.exp2((s - top) * factor) for s in parts]
        total = functools.reduce(jnp.add, [jnp.sum(e, axis=1, keepdims=True) for e in parts])
        inverse = 1.0 / total
        one, two = inverse[:tok], inverse[tok:] * lam
        raw = None
        for (first, size), e in zip(spans, parts):
            mixing = (e[:tok] * one - e[tok:] * two).astype(jnp.bfloat16)
            term = jnp.dot(mixing, rx[2, j, first : first + size, :], preferred_element_type=jnp.float32)
            raw = term if raw is None else raw + term
        scaled = raw * lax.rsqrt(jnp.mean(raw * raw, axis=1, keepdims=True) + EPSILON)
        result = (scaled * hg_ref[...] * OUT_SCALE).astype(jnp.bfloat16)

        @pl.when(i == me)
        def _():
            hrx[j, :, pl.ds(pl.multiple_of(me * width, width), width)] = result

        @pl.when(i != me)
        def _():
            heads_out[j, i] = result
            heads_to(j, i).start()

    def forward(stage):
        if stage < CHUNKS:
            for xo in range(1, nx):
                weight_x_in(xo, stage).wait_recv()
                if ways > 1:
                    weight_y(xo, stage).start()
                if cores > 1:
                    weight_core(xo, stage, 0).start()
        elif ways > 1:
            for xo in range(1, nx):
                weight_y_in(xo, stage - CHUNKS).wait_recv()
                if cores > 1:
                    weight_core(xo, stage - CHUNKS, 1).start()

    for table in tables:
        table.wait()
    for j in range(local_heads):
        lam = lam_ref[me * local_heads + j]
        for t, (target, gain) in enumerate(((rot_k, kg_ref), (rot_q, qg_ref), (None, None))):
            own_rows(t, j).wait()
            for off in range(1, n):
                rows_from(t, j, off).wait_recv()
            if target is not None:
                target[...] = norm_rotate(rx[t, j], jnp.concatenate([gain[...]] * 2, axis=1))
        for g in range(groups):
            if per_group == 1:
                query_block(j, g, g, lam)
            else:
                def step(b, carry, j=j, g=g, lam=lam):
                    query_block(j, g, g * per_group + b, lam)
                    return carry
                lax.fori_loop(0, per_group, step, 0)
        for stage in range(2 * CHUNKS):
            if j == min(stage, local_heads - 1):
                forward(stage)

    own_weight.wait()
    if cores > 1:
        for xo in range(nx):
            for r in range(CHUNKS):
                for way in range(ways):
                    weight_core_in(xo, r, way).wait_recv()

    for j in range(local_heads):
        for off in range(1, n):
            heads_from(j, off).wait_recv()
        rows = hrx[j]
        for index in range(n_dp):
            matching = jnp.concatenate(
                [wfull[index, pl.ds((s * local_heads + j) * width, width), :] for s in range(n)], axis=0
            )
            term = jnp.dot(rows, matching, preferred_element_type=jnp.float32)
            span = slice(index * cols, (index + 1) * cols)
            if j:
                term = total[:, span] + term
            if j == local_heads - 1:
                out_ref[0, :, span] = term.astype(out_ref.dtype)
            else:
                total[:, span] = term

    for j in range(local_heads):
        for off in range(1, n):
            for t in range(3):
                rows_to(t, j, off).wait_send()
            heads_to(j, sp_peer(off)).wait_send()
    for r in range(CHUNKS):
        for xo in range(nx):
            if xo:
                weight_x(xo, r).wait_send()
                if ways > 1:
                    weight_y(xo, r).wait_send()
            if cores > 1:
                for way in range(ways):
                    weight_core(xo, r, way).wait_send()


def local(n, n_dp, n_grp, query_rows, key_rows, value_rows, query_gain, key_gain, lambdas, head_gain, out_weight):
    tok = query_rows.shape[1]
    head_size = query_gain.shape[0]
    width = head_gain.shape[0]
    local_heads = lambdas.shape[0] // n
    length = tok * n
    depth, cols = out_weight.shape
    cores = CORES if n_dp % CORES == 0 else 1
    nx = n_dp // cores
    cosine, sine = rotation_tables(length, head_size)
    anywhere = pl.BlockSpec(memory_space=pl.ANY)
    vmem = pl.BlockSpec(memory_space=pltpu.VMEM)
    dma = pltpu.SemaphoreType.DMA
    return pl.pallas_call(
        functools.partial(kernel, n, n_dp, n_grp, head_size),
        out_shape=jax.ShapeDtypeStruct((1, tok, n_dp * cols), jnp.bfloat16),
        in_specs=[anywhere] * 3
        + [vmem, vmem, pl.BlockSpec(memory_space=pltpu.SMEM), vmem, anywhere, anywhere, anywhere],
        out_specs=vmem,
        scratch_shapes=[
            pltpu.VMEM((tok, n_dp * cols), jnp.float32),
            pltpu.VMEM((3, local_heads, length, width), jnp.bfloat16),
            pltpu.VMEM((length, width), jnp.bfloat16),
            pltpu.VMEM((length, width), jnp.bfloat16),
            pltpu.VMEM((local_heads, n, tok, width), jnp.bfloat16),
            pltpu.VMEM((local_heads, tok, n * width), jnp.bfloat16),
            pltpu.VMEM((n_dp, depth, cols), jnp.bfloat16),
            dma((3, local_heads, n)),
            dma((3, local_heads, n)),
            dma((local_heads, n)),
            dma((local_heads, n)),
            dma((nx, CHUNKS)),
            dma((nx, CHUNKS)),
            dma((nx, CHUNKS)),
            dma((nx, CHUNKS)),
            dma((nx, CHUNKS, WAYS)),
            dma((nx, CHUNKS, WAYS)),
            dma(()),
            pltpu.VMEM((length, width), jnp.float32),
            pltpu.VMEM((length, width), jnp.float32),
            dma((2,)),
        ],
        compiler_params=pltpu.CompilerParams(
            collective_id=0, has_side_effects=True, vmem_limit_bytes=56 * 1024 * 1024
        ),
    )(
        query_rows, key_rows, value_rows,
        query_gain[None, :], key_gain[None, :], lambdas, head_gain[None, :],
        out_weight, jnp.asarray(cosine), jnp.asarray(sine),
    )


def solution(mesh):
    rows = P(("grp", "dp"), "sp", None)
    return jax.shard_map(
        functools.partial(local, mesh.shape["sp"], mesh.shape["dp"], mesh.shape["grp"]),
        mesh=mesh,
        in_specs=(rows, rows, rows, P(), P(), P(), P(), P(None, "dp")),
        out_specs=rows,
        check_vma=False,
    )
```
